32 devices in a mesh: sp: 8 (over z, x), tp: 4 (over y, core).
Axes of the slice: x: 2, y: 2, z: 4, core: 2. Of those that a mesh axis runs over, the one named last changes fastest.
Arguments:
- moe_input: bfloat16 [1024, 2048], P('sp'), may hold values from -6 to 6
- out_grad: bfloat16 [1024, 2048], P('sp'), may hold values from -6 to 6
- routes: int32 [1024, 2], P('sp'), may hold values from 0 to 3, all different within a row; in each aligned block of 128 rows (0 to 127, 128 to 255, ...) at most 96 rows name the same one
- route_weights: float32 [1024, 2], P('sp'), may hold values from 0.2 to 1
- gate_cols: bfloat16 [2048, 14336], P(None, ('sp', 'tp')), may hold values from -0.125 to 0.125
- up_cols: bfloat16 [2048, 14336], P(None, ('sp', 'tp')), may hold values from -0.125 to 0.125
- down_rows: bfloat16 [14336, 2048], P(('sp', 'tp')), may hold values from -0.09375 to 0.09375
- out_proj: bfloat16 [2048, 512], P(None, 'tp'), may hold values from -0.25 to 0.25
- conv_out: bfloat16 [1024, 512], P('sp', 'tp'), may hold values from -6 to 6
- gate_b: bfloat16 [1024, 512], P('sp', 'tp'), may hold values from -6 to 6
- gate_c: bfloat16 [1024, 512], P('sp', 'tp'), may hold values from -6 to 6
- hidden_h: bfloat16 [1024, 512], P('sp', 'tp'), may hold values from -6 to 6
- conv_taps: float32 [3, 512], P(None, 'tp'), may hold values from -3.5 to 3.5
Outputs:
- grad_gate: bfloat16 [2048, 14336], P(None, ('sp', 'tp'))
- grad_up: bfloat16 [2048, 14336], P(None, ('sp', 'tp'))
- grad_down: bfloat16 [14336, 2048], P(('sp', 'tp'))
- grad_proj: float32 [2048, 512], P('sp', 'tp')
- grad_hidden: bfloat16 [1024, 512], P('sp', 'tp')
- grad_gate_b: bfloat16 [1024, 512], P('sp', 'tp')
- grad_gate_c: bfloat16 [1024, 512], P('sp', 'tp')
The draws below stay inside these ranges and needn't reach their ends.
Inputs may be any that keep to these rules, and one draw needn't show every extreme that they name: `routes`: each row names 2 different experts. Among the rows of one device no expert is named more than 96 times, a bound that some block reaches.
All inputs are finite; a program needn't handle non-finite values.
Results may differ from the reference program's by a relative error of at most 0.01.
Values may be sent and summed in bfloat16 or wider, within the bound.
No kernel may reach another device: no remote copies, remote signals or barrier semaphores. Data moves between devices by JAX's collectives and lax.ppermute only.
A program may use at most 128 MiB of HBM per device.

```python
import math
from functools import partial
import jax
import jax.numpy as jnp
import numpy as np
from jax import lax

D = 2048
FF = 3584
CW = 512
KERNEL = 3
TOP = 2
TOK_DEV = 128
TOKENS = 1024
EXPERTS = 4
CAP = 96
N_SP = 8
N_TP = 4


def strengthened(drawn, own_key, source, target, blocks, factor):
    def block_of(position):
        return (jnp.arange(drawn.shape[position]) // (drawn.shape[position] // blocks)).reshape((-1,) + (1,) * (drawn.ndim - 1 - position))

    first = jax.random.permutation(own_key, blocks)[block_of(target)]
    second = (block_of(target) + blocks // 2) % blocks
    return jnp.where((block_of(source) == first) | (block_of(source) == second), factor * drawn, drawn)


def shard_levels(own_key, shape, split, least, high):
    def one(position, parts):
        steps = jax.random.uniform(jax.random.fold_in(jax.random.fold_in(own_key, 6), position), (parts,), jnp.float32, least / len(split), high / len(split))
        return jnp.repeat(jnp.exp(steps), shape[position] // parts).reshape((-1,) + (1,) * (len(shape) - position - 1))

    factor_of = one(*split[0])
    for cut in split[1:]:
        factor_of = factor_of * one(*cut)
    return factor_of


def assign_block(stream_key, own, number, rows, number_of, top, bound, slope):
    sequence = jax.random.permutation(stream_key, number_of)
    packed, common = load_shares(number_of, rows * top, bound, slope, True), load_shares(number_of, rows * top, bound, slope, False)
    places = jnp.arange(number_of)

    def named(sizes, offset_by):
        used = int((sizes > 0).sum())
        fixed = max(1, used // 4)
        shifted = fixed + (places - fixed + offset_by * (used - fixed)) % max(1, number_of - fixed)
        return jnp.zeros((number_of,), jnp.int32).at[sequence[jnp.where(places < fixed, places, shifted)]].set(jnp.asarray(sizes, jnp.int32))

    sizes = jnp.where(number % 4 == 0, named(packed, number // 4), named(common, number - number // 4 - 1))
    mixed = jax.random.permutation(jax.random.fold_in(own, 3), number_of)
    giver, taker = mixed[0:number_of // 2 * 2:2], mixed[1:number_of // 2 * 2:2]
    room = jnp.minimum(sizes[giver] - 1, bound - sizes[taker]) // 2
    room = jnp.where((giver == sequence[0]) | (taker == sequence[0]) | (sizes[taker] == 0), 0, jnp.maximum(room, 0))
    shifted = jax.random.randint(jax.random.fold_in(own, 4), (number_of // 2,), 0, 1 << 20) % (room + 1)
    sizes = sizes.at[giver].add(-shifted).at[taker].add(shifted)
    members = jnp.searchsorted(jnp.cumsum(sizes), jnp.arange(rows * top), side="right").astype(jnp.int32)
    grid = members.reshape(top, rows).T
    grid = grid[jax.random.permutation(jax.random.fold_in(own, 1), rows)]
    offset_by = jax.random.randint(jax.random.fold_in(own, 2), (rows, 1), 0, top)
    return jnp.take_along_axis(grid, (jnp.arange(top)[None, :] + offset_by) % top, axis=1)


def load_shares(number_of, total, reach, skew, full):
    loads = [(1 << 20) // math.isqrt(grade ** skew) + 1 for grade in range(1, number_of + 1)]
    largest = reach if full else min(reach, max(-(-total // number_of), total * loads[0] // sum(loads)))
    least = 1 if total - largest >= number_of - 1 else 0
    given, rest = [largest] + [least] * (number_of - 1), total - largest - least * (number_of - 1)
    while rest > 0:
        free = [i for i in range(1, number_of) if given[i] < largest] or [i for i in range(1, number_of) if given[i] < reach]
        mass, remaining = sum([loads[i] for i in free]), rest
        for i in free:
            addition = min(reach - given[i], max(1, remaining * loads[i] // mass), rest)
            given[i] = given[i] + addition
            rest = rest - addition
    return np.array(given)


def normal_values(key, dims, width, bound, split=(), kind=jnp.bfloat16):
    values = jax.random.normal(key, dims, jnp.float32) * width
    if len(split) > 0:
        values = shard_levels(key, dims, split, -0.22, 0.18) * values
    return jnp.clip(values, min=-bound, max=bound).astype(kind)


def noise_with(rng, dims, width, most, cuts, heavy, kind=jnp.bfloat16):
    values = width * jax.random.normal(rng, dims, jnp.float32)
    if cuts:
        values = values * shard_levels(rng, dims, cuts, -0.22, 0.18)
    return jnp.clip(strengthened(values, jax.random.fold_in(rng, 3), *heavy), -most, most).astype(kind)


def setup_inputs(seed: int = 0) -> dict:
    streams_of = jax.random.split(jax.random.key(seed), 14)
    moe_input = normal_values(streams_of[0], (TOKENS, D), 1.0, 6.0, ((0, 8),))
    out_grad = noise_with(streams_of[1], (TOKENS, D), 1.0, 6.0, ((0, 8),), (0, 1, 8, 2.0))
    routes_keys = jax.random.split(jax.random.fold_in(streams_of[2], 1), TOKENS // TOK_DEV)
    routes_turns = jax.random.permutation(jax.random.fold_in(streams_of[2], 3), TOKENS // TOK_DEV)
    routes = jax.vmap(lambda own, number: assign_block(jax.random.fold_in(streams_of[2], 2), own, number, TOK_DEV, EXPERTS, TOP, CAP, 2))(routes_keys, routes_turns).reshape((TOKENS, TOP))
    route_weights = jnp.clip(0.2 + 0.8 * jax.random.uniform(streams_of[3], (TOKENS, TOP), jnp.float32) ** shard_levels(streams_of[3], (TOKENS, TOP), ((0, 8),), -0.2, 0.2), 0.2, 1.0)
    gate_cols = normal_values(streams_of[4], (D, EXPERTS * FF), D ** -0.5, 0.125, ((1, 32),))
    up_cols = normal_values(streams_of[5], (D, EXPERTS * FF), D ** -0.5, 0.125, ((1, 32),))
    down_rows = normal_values(streams_of[6], (EXPERTS * FF, D), FF ** -0.5, 0.09375, ((0, 32),))
    out_proj = normal_values(streams_of[7], (D, CW), CW ** -0.5, 0.25, ((1, 4),))
    conv_out = normal_values(streams_of[8], (TOKENS, CW), 1.0, 6.0, ((0, 8), (1, 4)))
    gate_b = normal_values(streams_of[9], (TOKENS, CW), 1.0, 6.0, ((0, 8), (1, 4)))
    gate_c = normal_values(streams_of[10], (TOKENS, CW), 1.0, 6.0, ((0, 8), (1, 4)))
    hidden_h = normal_values(streams_of[11], (TOKENS, CW), 1.0, 6.0, ((0, 8), (1, 4)))
    conv_taps = normal_values(streams_of[12], (KERNEL, CW), KERNEL ** -0.5, 3.5, ((1, 4),), jnp.float32)
    return dict(moe_input=moe_input, out_grad=out_grad, routes=routes, route_weights=route_weights, gate_cols=gate_cols, up_cols=up_cols, down_rows=down_rows, out_proj=out_proj, conv_out=conv_out, gate_b=gate_b, gate_c=gate_c, hidden_h=hidden_h, conv_taps=conv_taps)


def slot_positions(route_block, experts, capacity):
    flat_ids = route_block.reshape(-1)
    one_hot = (flat_ids[:, None] == jnp.arange(experts, dtype=jnp.int32)[None, :]).astype(jnp.int32)
    earlier = jnp.cumsum(one_hot, axis=0) - one_hot
    ranked = jnp.sum(earlier * one_hot, axis=1)
    return (flat_ids * capacity + ranked).astype(jnp.int32)


def contract_rows(left_side, right_side):
    return lax.dot_general(left_side, right_side, (((0,), (0,)), ((), ())), preferred_element_type=jnp.float32)


def contract_cols(left_side, right_side):
    return lax.dot_general(left_side, right_side, (((1,), (1,)), ((), ())), preferred_element_type=jnp.float32)


def fill_table(slot_place, route_vals):
    return jnp.full((EXPERTS * CAP,), TOKENS * TOP, jnp.int32).at[slot_place].set(route_vals)


def reference(moe_input, out_grad, routes, route_weights, gate_cols, up_cols, down_rows, out_proj, conv_out, gate_b, gate_c, hidden_h, conv_taps):
    positions = jax.vmap(partial(slot_positions, experts=EXPERTS, capacity=CAP))(routes.reshape(N_SP, TOK_DEV, TOP))
    pair_ids = (jnp.arange(N_SP, dtype=jnp.int32)[:, None] * (TOK_DEV * TOP)
                + jnp.arange(TOK_DEV * TOP, dtype=jnp.int32)[None, :])
    tables = jax.vmap(fill_table)(positions, pair_ids)
    tables = jnp.transpose(tables.reshape(N_SP, EXPERTS, CAP), (1, 0, 2))
    scaled = (route_weights[:, :, None] * out_grad[:, None, :].astype(jnp.float32)).astype(jnp.bfloat16)
    scaled = scaled.reshape(TOKENS * TOP, D)
    zero_row = jnp.zeros((1, D), jnp.bfloat16)
    padded_x = jnp.concatenate([moe_input, zero_row], axis=0)
    padded_g = jnp.concatenate([scaled, zero_row], axis=0)
    unit_block = FF // (2 * N_TP)

    def expert_step(gathered, inputs):
        slot_table, expert_index = inputs
        route_rows = slot_table.reshape(-1)
        token_rows = route_rows // TOP
        rows_x = padded_x[token_rows]
        rows_g = padded_g[route_rows]
        w_gate = lax.dynamic_slice_in_dim(gate_cols, expert_index * FF, FF, 1)
        w_up = lax.dynamic_slice_in_dim(up_cols, expert_index * FF, FF, 1)
        w_down = lax.dynamic_slice_in_dim(down_rows, expert_index * FF, FF, 0)
        gate_pre = jnp.dot(rows_x, w_gate, preferred_element_type=jnp.float32)
        up_pre = jnp.dot(rows_x, w_up, preferred_element_type=jnp.float32)
        sigmoid_g = jax.nn.sigmoid(gate_pre)
        silu_g = gate_pre * sigmoid_g
        activation = (silu_g * up_pre).astype(jnp.bfloat16)
        grad_down_e = contract_rows(activation, rows_g).astype(jnp.bfloat16)
        d_act = contract_cols(rows_g, w_down)
        d_up = (d_act * silu_g).astype(jnp.bfloat16)
        d_gate = (d_act * up_pre * sigmoid_g * (1.0 + gate_pre * (1.0 - sigmoid_g))).astype(jnp.bfloat16)
        grad_gate_e = contract_rows(rows_x, d_gate).astype(jnp.bfloat16)
        grad_up_e = contract_rows(rows_x, d_up).astype(jnp.bfloat16)
        back_rows = jnp.zeros((route_rows.shape[0], D), jnp.float32)
        for half_index in range(2):
            running = jnp.zeros((route_rows.shape[0], D), jnp.float32)
            for quarter_index in range(N_TP):
                first_unit = (half_index * N_TP + quarter_index) * unit_block
                piece_sum = (contract_cols(d_gate[:, first_unit:first_unit + unit_block], w_gate[:, first_unit:first_unit + unit_block])
                             + contract_cols(d_up[:, first_unit:first_unit + unit_block], w_up[:, first_unit:first_unit + unit_block]))
                piece_sum = lax.optimization_barrier(piece_sum.astype(jnp.bfloat16))
                running = running + piece_sum.astype(jnp.float32)
            half_sum = lax.optimization_barrier(running.astype(jnp.bfloat16))
            back_rows = back_rows + half_sum.astype(jnp.float32)
        gathered = gathered.at[token_rows].add(back_rows)
        return gathered, (grad_gate_e, grad_up_e, grad_down_e)

    start_back = jnp.zeros((TOKENS + 1, D), jnp.float32)
    moe_back, stacked = lax.scan(expert_step, start_back, (tables, jnp.arange(EXPERTS, dtype=jnp.int32)))
    grad_gate = jnp.transpose(stacked[0], (1, 0, 2)).reshape(D, EXPERTS * FF)
    grad_up = jnp.transpose(stacked[1], (1, 0, 2)).reshape(D, EXPERTS * FF)
    grad_down = stacked[2].reshape(EXPERTS * FF, D)
    stream_grad = (out_grad.astype(jnp.float32) + moe_back[:TOKENS]).astype(jnp.bfloat16)
    branch = (gate_b.astype(jnp.float32) * conv_out.astype(jnp.float32)).astype(jnp.bfloat16)
    d_branch = jnp.dot(stream_grad, out_proj, preferred_element_type=jnp.float32)
    grad_proj = contract_rows(stream_grad, branch)
    grad_gate_b = (d_branch * conv_out.astype(jnp.float32)).astype(jnp.bfloat16)
    d_conv = d_branch * gate_b.astype(jnp.float32)
    extended = jnp.concatenate([d_conv, jnp.zeros((KERNEL - 1, CW), jnp.float32)], axis=0)
    d_input = jnp.zeros((TOKENS, CW), jnp.float32)
    for tap_index in range(KERNEL):
        offset = KERNEL - 1 - tap_index
        d_input = d_input + conv_taps[tap_index][None, :] * extended[offset:offset + TOKENS]
    grad_hidden = (d_input * gate_c.astype(jnp.float32)).astype(jnp.bfloat16)
    grad_gate_c = (d_input * hidden_h.astype(jnp.float32)).astype(jnp.bfloat16)
    return (grad_gate, grad_up, grad_down, grad_proj, grad_hidden, grad_gate_b, grad_gate_c)
```

```python
import jax
import jax.numpy as jnp
from jax import lax
from jax.sharding import PartitionSpec as P

BF = jnp.bfloat16
F32 = jnp.float32
BOTH = ("sp", "tp")


def dot(a, b, ca, cb):
    return lax.dot_general(a, b, (((ca,), (cb,)), ((), ())), preferred_element_type=F32)


def moved(block, dz=0, dx=0, dy=0, dc=0):
    sp, tp = lax.axis_size("sp"), lax.axis_size("tp")
    route = []
    for s in range(sp):
        for t in range(tp):
            s2 = s ^ (dz * 2 + dx)
            t2 = t ^ (dy * 2 + dc)
            route.append((s * tp + t, s2 * tp + t2))
    return lax.ppermute(block, BOTH, route)


def per_device(
    moe_input,
    out_grad,
    routes,
    route_weights,
    gate_cols,
    up_cols,
    down_rows,
    out_proj,
    conv_out,
    gate_b,
    gate_c,
    hidden_h,
    conv_taps,
):
    sp, tp = lax.axis_size("sp"), lax.axis_size("tp")
    experts = sp // 2
    tokens, width = moe_input.shape
    cap = 2 * (3 * tokens // sp)
    slots = experts * cap
    quarter = width // tp
    chans = conv_out.shape[1]
    s_me, t_me = lax.axis_index("sp"), lax.axis_index("tp")
    e_me, x_me = s_me // 2, s_me % 2
    u_me, v_me = t_me // 2, t_me % 2

    op_y = moved(out_proj, dy=1)
    op_half = jnp.concatenate([out_proj, op_y], axis=1)
    op_c = moved(op_half, dc=1)
    op_full = jnp.concatenate([op_half, op_c], axis=1)

    ids = (e_me ^ jnp.arange(experts, dtype=jnp.int32))[:, None]
    r0, r1 = routes[:, 0][None, :], routes[:, 1][None, :]
    w0, w1 = route_weights[:, 0][None, :], route_weights[:, 1][None, :]
    named = (r0 == ids) | (r1 == ids)
    before = (
        lax.broadcasted_iota(jnp.int32, (tokens, tokens), 0)
        < lax.broadcasted_iota(jnp.int32, (tokens, tokens), 1)
    ).astype(BF)
    rank = dot(named.astype(BF), before, 1, 0)
    slot_no = lax.broadcasted_iota(jnp.int32, (experts, cap, tokens), 1).astype(F32)
    hit = named[:, None, :] & (rank[:, None, :] == slot_no)
    pick = hit.astype(BF).reshape(slots, tokens)
    weight_of = jnp.where(r0 == ids, w0, w1)
    slot_weight = jnp.sum(
        jnp.where(hit, weight_of[:, None, :], 0.0), axis=2, keepdims=True
    ).reshape(slots, 1)

    branch = (gate_b.astype(F32) * conv_out.astype(F32)).astype(BF)
    own_x = lax.dynamic_slice_in_dim(moe_input, t_me * quarter, quarter, 1)
    own_g = lax.dynamic_slice_in_dim(out_grad, t_me * quarter, quarter, 1)
    send_x = dot(pick, jnp.concatenate([own_x, branch], axis=1), 1, 0).astype(BF)
    send_g = (dot(pick, own_g, 1, 0) * slot_weight).astype(BF)

    def over_experts(rows):
        pieces = [rows[:cap]]
        for d in range(1, experts):
            pieces.append(moved(rows[d * cap : (d + 1) * cap], dz=d))
        return pieces

    def in_plane(pieces):
        half = experts // 2
        a = jnp.concatenate(pieces[:half], axis=0)
        b = jnp.concatenate(pieces[half:], axis=0)
        ay = moved(a, dy=1)
        bx = moved(b, dx=1)
        a2 = jnp.stack([a, ay])
        ax = moved(a2, dx=1)
        b2 = jnp.stack([b, bx])
        by = moved(b2, dy=1)
        own = jnp.stack(
            [
                jnp.concatenate([a, b, ax[0], bx], axis=0),
                jnp.concatenate([ay, by[0], ax[1], by[1]], axis=0),
            ]
        )
        return own, moved(own, dc=1)

    def absolute(own, other):
        own = jnp.where(u_me == 0, own, own[::-1])
        other = jnp.where(u_me == 0, other, other[::-1])
        even = jnp.where(v_me == 0, own, other)
        odd = jnp.where(v_me == 0, other, own)
        return jnp.concatenate([even[0], odd[0], even[1], odd[1]], axis=1)

    xb, xb_c = in_plane(over_experts(send_x))
    g, g_c = in_plane(over_experts(send_g))
    rows_x = absolute(xb[:, :, :quarter], xb_c[:, :, :quarter])
    rows_g = absolute(g, g_c)
    rows_b = jnp.concatenate(
        [xb[0, :, quarter:], xb[1, :, quarter:], xb_c[0, :, quarter:], xb_c[1, :, quarter:]],
        axis=1,
    )

    v_gate = dot(gate_cols, op_full, 0, 0).astype(BF)
    v_up = dot(up_cols, op_full, 0, 0).astype(BF)

    gate_pre = dot(rows_x, gate_cols, 1, 0)
    up_pre = dot(rows_x, up_cols, 1, 0)
    sig = jax.nn.sigmoid(gate_pre)
    silu = gate_pre * sig
    act = (silu * up_pre).astype(BF)
    d_act = dot(rows_g, down_rows, 1, 1)
    d_up = (d_act * silu).astype(BF)
    d_gate = (d_act * up_pre * sig * (1.0 + gate_pre * (1.0 - sig))).astype(BF)

    def back(lo, hi):
        return dot(d_gate, v_gate[:, lo:hi], 1, 0) + dot(d_up, v_up[:, lo:hi], 1, 0)

    pair = 2 * chans
    r_sent = moved(back(pair, 2 * pair).astype(BF), dc=1)
    r_own = back(0, pair) + r_sent.astype(F32)

    def plane_sum(p00, p10, p01, p11):
        x_in = moved(p10.astype(BF), dx=1)
        y_in = moved(p01.astype(BF), dy=1)
        d_in = moved(p11.astype(BF), dx=1, dy=1)
        return p00 + x_in.astype(F32) + y_in.astype(F32) + d_in.astype(F32)

    r_sum = plane_sum(
        r_own[:slots, :chans], r_own[slots:, :chans], r_own[:slots, chans:], r_own[slots:, chans:]
    ).astype(BF)
    home = jnp.concatenate(over_experts(r_sum), axis=0)

    h_gate = dot(d_gate, rows_b, 0, 0).astype(BF)
    h_up = dot(d_up, rows_b, 0, 0).astype(BF)

    def proj(lo, hi):
        return dot(gate_cols, h_gate[:, lo:hi], 1, 0) + dot(up_cols, h_up[:, lo:hi], 1, 0)

    q_sent = moved(proj(pair, 2 * pair).astype(BF), dc=1)
    q_own = proj(0, pair) + q_sent.astype(F32)
    q_base = dot(out_grad, branch, 0, 0)
    feats = width // sp
    q_own = q_own.reshape(experts, 2, feats, pair)
    q_base = q_base.reshape(experts, 2, feats, chans)

    def of_half(arr, x):
        return lax.dynamic_index_in_dim(arr, x, 1, keepdims=False)

    mine, theirs = of_half(q_own, x_me), of_half(q_own, 1 - x_me)
    q_sum = plane_sum(
        mine[..., :chans] + of_half(q_base, x_me),
        theirs[..., :chans] + of_half(q_base, 1 - x_me),
        mine[..., chans:],
        theirs[..., chans:],
    )
    grad_proj = lax.dynamic_index_in_dim(q_sum, e_me, 0, keepdims=False)
    q_send = q_sum.astype(BF)
    for d in range(1, experts):
        block = lax.dynamic_index_in_dim(q_send, e_me ^ d, 0, keepdims=False)
        grad_proj = grad_proj + moved(block, dz=d).astype(F32)

    grad_down = dot(act, rows_g, 0, 0).astype(BF)
    grad_gate = dot(rows_x, d_gate, 0, 0).astype(BF)
    grad_up = dot(rows_x, d_up, 0, 0).astype(BF)

    d_branch = dot(out_grad, out_proj, 1, 0) + dot(pick, home, 0, 0)
    grad_gate_b = (d_branch * conv_out.astype(F32)).astype(BF)
    d_conv = d_branch * gate_b.astype(F32)
    taps = conv_taps.shape[0]
    reach = taps - 1
    route = [(i * tp + t, (i - 1) * tp + t) for i in range(1, sp) for t in range(tp)]
    next_rows = lax.ppermute(d_conv[:reach], BOTH, route)
    extended = jnp.concatenate([d_conv, next_rows], axis=0)
    d_input = jnp.zeros_like(d_conv)
    for tap in range(taps):
        offset = reach - tap
        d_input = d_input + conv_taps[tap][None, :] * extended[offset : offset + tokens]
    grad_hidden = (d_input * gate_c.astype(F32)).astype(BF)
    grad_gate_c = (d_input * hidden_h.astype(F32)).astype(BF)
    return (grad_gate, grad_up, grad_down, grad_proj, grad_hidden, grad_gate_b, grad_gate_c)


def solution(mesh):
    placed = (
        P("sp", None),
        P("sp", None),
        P("sp", None),
        P("sp", None),
        P(None, ("sp", "tp")),
        P(None, ("sp", "tp")),
        P(("sp", "tp"), None),
        P(None, "tp"),
        P("sp", "tp"),
        P("sp", "tp"),
        P("sp", "tp"),
        P("sp", "tp"),
        P(None, "tp"),
    )
    return jax.shard_map(
        per_device,
        mesh=mesh,
        in_specs=placed,
        out_specs=(
            P(None, ("sp", "tp")),
            P(None, ("sp", "tp")),
            P(("sp", "tp"), None),
            P("sp", "tp"),
            P("sp", "tp"),
            P("sp", "tp"),
            P("sp", "tp"),
        ),
        check_vma=False,
    )
```
